32 devices in a mesh: sp: 4 (over z), fs: 4 (over y, x), tp: 2 (over core).
Axes of the slice: x: 2, y: 2, z: 4, core: 2. Of those that a mesh axis runs over, the one named last changes fastest.
Arguments:
- tokens: bfloat16 [4, 512, 2048], P('fs', ('sp', 'tp')), may hold values from -6 to 6
- norm_gain: float32 [2048], replicated, may hold values from 0.1 to 1.9
- gla_query_weight: bfloat16 [2048, 512], P('sp', 'tp'), may hold values from -0.125 to 0.125
- gla_key_weight: bfloat16 [2048, 512], P('sp', 'tp'), may hold values from -0.125 to 0.125
- gla_value_weight: bfloat16 [2048, 1024], P('sp', 'tp'), may hold values from -0.125 to 0.125
- decay_down: bfloat16 [2048, 32], P('sp'), may hold values from -0.125 to 0.125
- decay_up: bfloat16 [32, 512], P(None, 'tp'), may hold values from -1 to 1
- decay_bias: float32 [512], P('tp'), may hold values from 0.5 to 12
- head_gain: float32 [128], replicated, may hold values from 0.1 to 1.9
- window_query_weight: bfloat16 [2048, 1024], P('sp', 'tp'), may hold values from -3 to 3
- window_key_weight: bfloat16 [2048, 256], P('sp', 'tp'), may hold values from -3 to 3
- window_value_weight: bfloat16 [2048, 256], P('sp', 'tp'), may hold values from -0.125 to 0.125
- sink_logit: float32 [16], P('tp'), may hold values from 3 to 7
- gla_output_weight: bfloat16 [1024, 2048], P('tp', 'sp'), may hold values from -0.125 to 0.125
- window_output_weight: bfloat16 [1024, 2048], P('tp', 'sp'), may hold values from -0.125 to 0.125
Outputs:
- mixed: bfloat16 [4, 512, 2048], P('fs', ('sp', 'tp'))
The draws below stay inside these ranges and needn't reach their ends.
All inputs are finite; a program needn't handle non-finite values.
Results may differ from the reference program's by a relative error of at most 0.013.
Values may be sent and summed in bfloat16 or wider, within the bound.
A program may use at most 64 MiB of HBM per device.

```python
import jax
import jax.numpy as jnp
from jax import lax

D = 2048
GLA_HEADS = 8
KEY_DIM = 64
VALUE_DIM = 128
RANK = 32
SWA_HEADS = 16
KV_HEADS = 4
HEAD_DIM = 64
WINDOW = 128
SPAN = 64
SEQS = 4
LEN = 512


def gain_values(key):
    normal_draw = jax.random.normal(jax.random.fold_in(key, 11), (D,), jnp.float32)
    return 1.0 + 0.18 * jnp.clip(normal_draw, -5.0, 5.0)


def drawn_weight(key, salt_value, columns):
    raw_draw = jax.random.normal(jax.random.fold_in(key, salt_value), (D, columns), jnp.float32)
    raw_draw = jnp.clip(raw_draw, -6.0, 6.0) / jnp.sqrt(float(D))
    return raw_draw


def draw_window_query_weight(key, part):
    return drawn_weight(key, 16, SWA_HEADS * HEAD_DIM).astype(jnp.bfloat16)


def draw_window_key_weight(key, part):
    return drawn_weight(key, 17, KV_HEADS * HEAD_DIM).astype(jnp.bfloat16)


def draw_norm_gain(key, part):
    return gain_values(key)


def draw_tokens(key, part):
    base_draw = jax.random.normal(jax.random.fold_in(key, 21), (SEQS, LEN, D), jnp.float32)
    base_draw = jnp.clip(base_draw, -6.0, 6.0)
    return base_draw.astype(jnp.bfloat16)


def block_scale(stream_key, extent, split, smallest, high):
    level = 1.0
    for dim, blocks in split:
        steps = jax.random.uniform(jax.random.fold_in(jax.random.fold_in(stream_key, 6), dim), (blocks,), jnp.float32, smallest / len(split), high / len(split))
        level = level * jnp.repeat(jnp.exp(steps), extent[dim] // blocks).reshape((-1,) + (1,) * (len(extent) - 1 - dim))
    return level


def gaussian(own_key, extent, deviation, limit, pieces=(), held_as=jnp.bfloat16):
    values = deviation * jax.random.normal(own_key, extent, jnp.float32)
    if pieces:
        values = values * block_scale(own_key, extent, pieces, -0.22, 0.18)
    return jnp.clip(values, -limit, limit).astype(held_as)


def setup_inputs(seed: int = 0) -> dict:
    streams_of = jax.random.split(jax.random.key(seed), 16)
    tokens = draw_tokens(jax.random.fold_in(streams_of[15], 71), 0)
    norm_gain = draw_norm_gain(jax.random.fold_in(streams_of[15], 71), 0)
    gla_query_weight = gaussian(streams_of[2], (D, GLA_HEADS * KEY_DIM), D ** -0.5, 0.125, ((0, 4), (1, 2)))
    gla_key_weight = gaussian(streams_of[3], (D, GLA_HEADS * KEY_DIM), D ** -0.5, 0.125, ((0, 4), (1, 2)))
    gla_value_weight = gaussian(streams_of[4], (D, GLA_HEADS * VALUE_DIM), D ** -0.5, 0.125, ((0, 4), (1, 2)))
    decay_down = gaussian(streams_of[5], (D, RANK), D ** -0.5, 0.125, ((0, 4),))
    decay_up = gaussian(streams_of[6], (RANK, GLA_HEADS * KEY_DIM), RANK ** -0.5, 1.0, ((1, 2),))
    decay_bias = jnp.clip(0.5 + 11.5 * jax.random.uniform(streams_of[7], (GLA_HEADS * KEY_DIM,), jnp.float32) ** block_scale(streams_of[7], (GLA_HEADS * KEY_DIM,), ((0, 2),), -0.2, 0.2), 0.5, 12.0)
    head_gain = jnp.clip(1.0 + 0.18 * jax.random.normal(streams_of[8], (VALUE_DIM,), jnp.float32), 0.1, 1.9)
    window_query_weight = draw_window_query_weight(jax.random.fold_in(streams_of[15], 71), 0)
    window_key_weight = draw_window_key_weight(jax.random.fold_in(streams_of[15], 71), 0)
    window_value_weight = gaussian(streams_of[11], (D, KV_HEADS * HEAD_DIM), D ** -0.5, 0.125, ((0, 4), (1, 2)))
    sink_logit = jnp.clip(3.0 + 4.0 * jax.random.uniform(streams_of[12], (SWA_HEADS,), jnp.float32) ** block_scale(streams_of[12], (SWA_HEADS,), ((0, 2),), -0.2, 0.2), 3.0, 7.0)
    gla_output_weight = gaussian(streams_of[13], (GLA_HEADS * VALUE_DIM, D), (GLA_HEADS * VALUE_DIM + SWA_HEADS * HEAD_DIM) ** -0.5, 0.125, ((0, 2), (1, 4)))
    window_output_weight = gaussian(streams_of[14], (SWA_HEADS * HEAD_DIM, D), (GLA_HEADS * VALUE_DIM + SWA_HEADS * HEAD_DIM) ** -0.5, 0.125, ((0, 2), (1, 4)))
    return {"tokens": tokens, "norm_gain": norm_gain, "gla_query_weight": gla_query_weight, "gla_key_weight": gla_key_weight, "gla_value_weight": gla_value_weight, "decay_down": decay_down, "decay_up": decay_up, "decay_bias": decay_bias, "head_gain": head_gain, "window_query_weight": window_query_weight, "window_key_weight": window_key_weight, "window_value_weight": window_value_weight, "sink_logit": sink_logit, "gla_output_weight": gla_output_weight, "window_output_weight": window_output_weight}


EPS = 1e-06
SOFTMAX_TEMPER = 16.0
HIGH = lax.Precision.HIGHEST

def rms_rows(values, gain):
    mean_square = lax.optimization_barrier(jnp.mean(values * values, axis=-1, keepdims=True))
    return values * lax.rsqrt(mean_square + EPS) * gain

def block_terms(query_rows, key_rows, value_rows, log_decay_rate, block_len):
    seq_len, head_count, key_width = query_rows.shape
    value_width = value_rows.shape[-1]
    block_count = seq_len // block_len
    q_scaled = query_rows.reshape(block_count, block_len, head_count, key_width) * key_width ** (-0.5)
    k_blocks = key_rows.reshape(block_count, block_len, head_count, key_width)
    v_blocks = value_rows.reshape(block_count, block_len, head_count, value_width)
    within = jnp.cumsum(log_decay_rate.reshape(block_count, block_len, head_count, key_width), axis=1)
    block_total = within[:, -1]
    q_dec = q_scaled * jnp.exp(within)
    k_dec = k_blocks * jnp.exp(-within)
    k_end = k_blocks * jnp.exp(block_total[:, None] - within)
    causal = jnp.tril(jnp.ones((block_len, block_len), dtype=bool))
    scores = jnp.einsum('nihd,njhd->nhij', q_dec, k_dec, precision=HIGH)
    scores = jnp.where(causal, scores, 0.0)
    local_out = jnp.einsum('nhij,njhe->nihe', scores, v_blocks, precision=HIGH)
    update = jnp.einsum('njhd,njhe->nhde', k_end, v_blocks, precision=HIGH)

    def advance(carried, inputs):
        update_in, decay_in = inputs
        return (decay_in[..., None] * carried + update_in, carried)
    start_state = jnp.zeros((head_count, key_width, value_width), jnp.float32)
    last_state, entering = lax.scan(advance, start_state, (update, jnp.exp(block_total)))
    return (q_dec, local_out, entering, last_state, block_total)

def window_band_mask(block_count, block_len, offset):
    query_pos = jnp.arange(block_len)[:, None] + block_len
    key_pos = jnp.arange(2 * block_len)[None, :]
    distance = query_pos - key_pos
    inside = (distance >= 0) & (distance < block_len)
    global_key = offset + jnp.arange(block_count)[:, None, None] * block_len - block_len + key_pos[None]
    return inside[None] & (global_key >= 0)

def window_attend(query_blocks, key_band, value_band, valid, sinks):
    scores = jnp.einsum('nqhgd,nkhd->nhgqk', query_blocks.astype(jnp.float32), key_band.astype(jnp.float32))
    scores = scores * HEAD_DIM ** (-0.5)
    scores = jnp.where(valid[:, None, None], scores, -1e+30)
    sink_term = sinks[None, :, :, None, None]
    top = jnp.maximum(lax.optimization_barrier(jnp.max(scores, axis=-1, keepdims=True)), sink_term)
    expo = jnp.exp(scores - top)
    denom = lax.optimization_barrier(jnp.sum(expo, axis=-1, keepdims=True)) + jnp.exp(sink_term - top)
    weights = (expo / denom).astype(jnp.bfloat16)
    attended = jnp.einsum('nhgqk,nkhd->nqhgd', weights.astype(jnp.float32), value_band.astype(jnp.float32))
    return attended.astype(jnp.bfloat16)

def reference(tokens, norm_gain, gla_query_weight, gla_key_weight, gla_value_weight, decay_down, decay_up, decay_bias, head_gain, window_query_weight, window_key_weight, window_value_weight, sink_logit, gla_output_weight, window_output_weight):

    def one_sequence(seq_rows):
        seq_len = seq_rows.shape[0]
        normed = rms_rows(seq_rows.astype(jnp.float32), norm_gain).astype(jnp.bfloat16)

        def project(weight):
            return jnp.dot(normed, weight, preferred_element_type=jnp.float32).astype(jnp.bfloat16)
        gla_query = project(gla_query_weight)
        gla_key = project(gla_key_weight)
        gla_value = project(gla_value_weight)
        low_rank = project(decay_down)
        gate_logit_values = jnp.dot(low_rank, decay_up, preferred_element_type=jnp.float32) + decay_bias
        log_decay_rate = jax.nn.log_sigmoid(gate_logit_values) / SOFTMAX_TEMPER
        q_dec, local_out, entering, last_state, block_total = block_terms(gla_query.astype(jnp.float32).reshape(seq_len, GLA_HEADS, KEY_DIM), gla_key.astype(jnp.float32).reshape(seq_len, GLA_HEADS, KEY_DIM), gla_value.astype(jnp.float32).reshape(seq_len, GLA_HEADS, VALUE_DIM), log_decay_rate.reshape(seq_len, GLA_HEADS, KEY_DIM), SPAN)
        gla_out = local_out + jnp.einsum('nihd,nhde->nihe', q_dec, entering, precision=HIGH)
        gla_out = gla_out.reshape(seq_len, GLA_HEADS, VALUE_DIM)
        gla_hidden = rms_rows(gla_out, head_gain).astype(jnp.bfloat16).reshape(seq_len, GLA_HEADS * VALUE_DIM)
        window_query = project(window_query_weight)
        sliding_key = project(window_key_weight)
        window_value = project(window_value_weight)
        block_count = seq_len // WINDOW
        group_size = SWA_HEADS // KV_HEADS
        query_blocks = window_query.reshape(block_count, WINDOW, KV_HEADS, group_size, HEAD_DIM)

        def banded(rows):
            blocks = rows.reshape(block_count, WINDOW, KV_HEADS, HEAD_DIM)
            earlier = jnp.concatenate([jnp.zeros_like(blocks[:1]), blocks[:-1]], axis=0)
            return jnp.concatenate([earlier, blocks], axis=1)
        valid = window_band_mask(block_count, WINDOW, 0)
        sinks = sink_logit.reshape(KV_HEADS, group_size)
        window_hidden = window_attend(query_blocks, banded(sliding_key), banded(window_value), valid, sinks)
        window_hidden = window_hidden.reshape(seq_len, SWA_HEADS * HEAD_DIM)
        total = jnp.dot(gla_hidden, gla_output_weight, preferred_element_type=jnp.float32)
        total = total + jnp.dot(window_hidden, window_output_weight, preferred_element_type=jnp.float32)
        return total.astype(jnp.bfloat16)
    return lax.map(one_sequence, tokens)
```

```python
import jax
import jax.numpy as jnp
from jax import lax
from jax.sharding import PartitionSpec as P

KEY_DIM = 64
VALUE_DIM = 128
SWA_HEADS = 16
KV_HEADS = 4
HEAD_DIM = 64
WINDOW = 128
SPAN = 64

EPS = 1e-06
SOFTMAX_TEMPER = 16.0
BF = jnp.bfloat16
F32 = jnp.float32


def rms_rows(values, gain):
    mean_square = jnp.mean(values * values, axis=-1, keepdims=True)
    return values * lax.rsqrt(mean_square + EPS) * gain


def quarter(weight, along):
    width = weight.shape[along] // lax.axis_size("fs")
    return lax.dynamic_slice_in_dim(weight, lax.axis_index("fs") * width, width, along)


def shared(weight, heads):
    group = SWA_HEADS // KV_HEADS
    first = (lax.axis_index("fs") * heads) // group
    count = max(1, heads // group)
    return lax.dynamic_slice_in_dim(weight, first * HEAD_DIM, count * HEAD_DIM, 1)


def dot(spec, a, b):
    return jnp.einsum(spec, a.astype(BF), b.astype(BF), preferred_element_type=F32)


def per_device(
    tokens,
    norm_gain,
    gla_query_weight,
    gla_key_weight,
    gla_value_weight,
    decay_down,
    decay_up,
    decay_bias,
    head_gain,
    window_query_weight,
    window_key_weight,
    window_value_weight,
    sink_logit,
    gla_output_weight,
    window_output_weight,
):
    fs, tp, sp = (lax.axis_size(n) for n in ("fs", "tp", "sp"))
    me = lax.axis_index("sp")
    heads = sink_logit.shape[0] // fs
    maps = [
        quarter(gla_value_weight, 1),
        quarter(window_query_weight, 1),
        quarter(gla_query_weight, 1),
        quarter(gla_key_weight, 1),
        shared(window_key_weight, heads),
        shared(window_value_weight, heads),
        decay_down,
    ]
    widths = [m.shape[1] for m in maps]
    w_in = lax.all_gather(jnp.concatenate(maps, 1), "sp", axis=0, tiled=True)
    w_out = lax.all_gather(
        jnp.concatenate([quarter(gla_output_weight, 0), quarter(window_output_weight, 0)], 0), "sp"
    )
    normed = rms_rows(tokens[0].astype(F32), norm_gain).astype(BF)
    normed = lax.all_gather(normed, ("fs", "tp"), axis=0, tiled=True)
    rows = normed.shape[0] // fs
    proj = jnp.dot(normed, w_in, preferred_element_type=F32).astype(BF)
    parts = []
    at = 0
    for w in widths:
        parts.append(proj[:, at : at + w])
        at += w
    gv, wq, gq, gk, wk, wv, low = parts
    up = quarter(decay_up, 1)
    logits = jnp.dot(low, up, preferred_element_type=F32) + quarter(decay_bias, 0)
    rate = jax.nn.log_sigmoid(logits) / SOFTMAX_TEMPER

    gh = gq.shape[1] // KEY_DIM
    nb = rows // SPAN
    q = gq.astype(F32).reshape(fs, nb, SPAN, gh, KEY_DIM) * KEY_DIM**-0.5
    k = gk.astype(F32).reshape(fs, nb, SPAN, gh, KEY_DIM)
    v = gv.reshape(fs, nb, SPAN, gh, VALUE_DIM)
    tri = jnp.tril(jnp.ones((SPAN, SPAN), F32))
    within = jnp.cumsum(rate.reshape(fs, nb, SPAN, gh, KEY_DIM), axis=2)
    total = within[:, :, -1]
    q_dec = q * jnp.exp(within)
    k_dec = k * jnp.exp(-within)
    k_end = k * jnp.exp(total[:, :, None] - within)
    scores = dot("bnihd,bnjhd->bnhij", q_dec, k_dec)
    scores = jnp.where(tri > 0, scores, 0.0)
    local_out = dot("bnhij,bnjhe->bnihe", scores, v)
    update = dot("bnjhd,bnjhe->bnhde", k_end, v)
    state = jnp.zeros((fs, gh, KEY_DIM, VALUE_DIM), F32)
    entering = []
    for n in range(nb):
        entering.append(state)
        state = jnp.exp(total[:, n])[..., None] * state + update[:, n]
    entering = jnp.stack(entering, 1)
    span_decay = jnp.exp(jnp.sum(total, axis=1))
    packed = jnp.concatenate([state, span_decay[..., None]], -1)
    packed = lax.all_gather(packed, "sp")

    def step(position, subtotal):
        longer = packed[position, ..., -1:] * subtotal + packed[position, ..., :-1]
        return jnp.where(position < me, longer, subtotal)

    incoming = lax.fori_loop(0, sp - 1, step, jnp.zeros_like(state))
    before = jnp.cumsum(total, axis=1) - total
    entering = entering + jnp.exp(before)[..., None] * incoming[:, None]
    gla_out = local_out + dot("bnihd,bnhde->bnihe", q_dec, entering)
    gla_hidden = rms_rows(gla_out, head_gain).astype(BF).reshape(fs * rows, gh * VALUE_DIM)

    kvh = wk.shape[1] // HEAD_DIM
    per = heads // kvh
    wb = rows // WINDOW
    kv = jnp.concatenate([wk, wv], 1).reshape(fs, rows, -1)
    edge = lax.ppermute(kv[:, rows - WINDOW :], "sp", [(i, i + 1) for i in range(sp - 1)])
    band = jnp.concatenate([edge, kv], 1)
    band = jnp.stack(
        [band[:, i * WINDOW : (i + 2) * WINDOW] for i in range(wb)], 1
    ).reshape(fs, wb, 2 * WINDOW, 2, kvh, HEAD_DIM)
    qw = wq.reshape(fs, wb, WINDOW, kvh, per, HEAD_DIM)
    s = dot("bnqhgd,bnkhd->bnhgqk", qw, band[:, :, :, 0]) * HEAD_DIM**-0.5
    distance = jnp.arange(WINDOW)[:, None] + WINDOW - jnp.arange(2 * WINDOW)[None, :]
    where = me * rows + jnp.arange(wb)[:, None, None] * WINDOW - WINDOW + jnp.arange(2 * WINDOW)
    valid = ((distance >= 0) & (distance < WINDOW))[None] & (where >= 0)
    s = jnp.where(valid[None, :, None, None], s, -1e30)
    sink = quarter(sink_logit, 0).reshape(1, 1, kvh, per, 1, 1)
    top = jnp.maximum(jnp.max(s, -1, keepdims=True), sink)
    e = jnp.exp(s - top)
    weights = (e / (jnp.sum(e, -1, keepdims=True) + jnp.exp(sink - top))).astype(BF)
    hidden = dot("bnhgqk,bnkhd->bnqhgd", weights, band[:, :, :, 1]).astype(BF)
    hidden = hidden.reshape(fs * rows, heads * HEAD_DIM)

    both = jnp.concatenate([gla_hidden, hidden], 1)
    part = jnp.einsum("rk,skn->rsn", both, w_out, preferred_element_type=F32)
    part = part.reshape(fs * rows, -1)
    mixed = lax.psum_scatter(part, ("fs", "tp"), scatter_dimension=0, tiled=True)
    return mixed.astype(BF)[None]


def solution(mesh):
    in_specs = (
        P("fs", ("sp", "tp"), None),
        P(),
        P("sp", "tp"),
        P("sp", "tp"),
        P("sp", "tp"),
        P("sp", None),
        P(None, "tp"),
        P("tp"),
        P(),
        P("sp", "tp"),
        P("sp", "tp"),
        P("sp", "tp"),
        P("tp"),
        P("tp", "sp"),
        P("tp", "sp"),
    )
    out_specs = P("fs", ("sp", "tp"), None)
    return jax.shard_map(
        per_device, mesh=mesh, in_specs=in_specs, out_specs=out_specs, check_vma=False
    )
```

```python
import functools

import jax
import jax.numpy as jnp
from jax import lax
from jax.experimental import pallas as pl
from jax.experimental.pallas import tpu as pltpu
from jax.sharding import PartitionSpec as P

KEY_DIM = 64
VALUE_DIM = 128
SWA_HEADS = 16
KV_HEADS = 4
HEAD_DIM = 64
WINDOW = 128
SPAN = 64

EPS = 1e-06
SOFTMAX_TEMPER = 16.0
BF = jnp.bfloat16
F32 = jnp.float32


def rms_rows(values, gain):
    mean_square = jnp.mean(values * values, axis=-1, keepdims=True)
    return values * lax.rsqrt(mean_square + EPS) * gain


def quarter(weight, along):
    width = weight.shape[along] // lax.axis_size("fs")
    return lax.dynamic_slice_in_dim(weight, lax.axis_index("fs") * width, width, along)


def shared(weight, heads):
    group = SWA_HEADS // KV_HEADS
    first = (lax.axis_index("fs") * heads) // group
    count = max(1, heads // group)
    return lax.dynamic_slice_in_dim(weight, first * HEAD_DIM, count * HEAD_DIM, 1)


def nt(a, b):
    return lax.dot_general(a, b, (((1,), (1,)), ((), ())), preferred_element_type=F32)


def nn(a, b):
    return lax.dot_general(a, b, (((1,), (0,)), ((), ())), preferred_element_type=F32)


def tn(a, b):
    return lax.dot_general(a, b, (((0,), (0,)), ((), ())), preferred_element_type=F32)


def exact(a, b):
    return lax.dot_general(
        a, b, (((1,), (0,)), ((), ())), precision=lax.Precision.HIGHEST, preferred_element_type=F32
    )


def mixer_kernel(
    sizes,
    tok_ref,
    win_ref,
    low_ref,
    wout_ref,
    ngain_ref,
    up_ref,
    bias_ref,
    hgain_ref,
    sink_ref,
    out_ref,
    x_buf,
    w_buf,
    l_buf,
    o_buf,
    proj,
    edge_out,
    edge_in,
    state_out,
    state_in,
    local_out,
    q_far,
    hidden,
    half_out,
    half_in,
    half_own,
    piece_out,
    piece_in,
    piece_own,
    local_sem,
    tok_send,
    tok_recv,
    w_send,
    w_recv,
    l_send,
    l_recv,
    o_send,
    o_recv,
    edge_sem,
    state_send,
    state_recv,
    half_send,
    half_recv,
    piece_send,
    piece_recv,
):
    sp, fs, tp = sizes
    me = lax.axis_index("sp")
    f = lax.axis_index("fs")
    c = lax.axis_index("tp")
    plane = fs * tp
    mine = f * tp + c
    own = tok_ref.shape[0]
    rows = own * tp
    kc = win_ref.shape[0]
    MESH = pl.DeviceIdType.MESH

    def remote(src, dst, ssem, rsem, target):
        return pltpu.make_async_remote_copy(
            src_ref=src, dst_ref=dst, send_sem=ssem, recv_sem=rsem,
            device_id=target, device_id_type=MESH,
        )

    def w_rows(s):
        return w_buf.at[pl.ds(pl.multiple_of(s * kc, kc), kc)]

    def w_copy(s, way, first):
        target = {"sp": me + (1 if way == 0 else -1)}
        return remote(
            win_ref if first else w_rows(s), w_rows(s), w_send.at[way, s], w_recv.at[s], target
        )

    def l_copy(s, way, first):
        target = {"sp": me + (1 if way == 0 else -1)}
        return remote(
            low_ref if first else l_buf.at[s], l_buf.at[s], l_send.at[way, s], l_recv.at[s], target
        )

    def o_copy(s, way, first):
        target = {"sp": me + (1 if way == 0 else -1)}
        return remote(
            wout_ref if first else o_buf.at[s], o_buf.at[s], o_send.at[way, s], o_recv.at[s], target
        )

    def tok_rows(i):
        return x_buf.at[pl.ds(pl.multiple_of(i * own, own), own)]

    def tok_copy(d, peer, sender):
        return remote(
            tok_ref, tok_rows(sender), tok_send.at[d - 1], tok_recv.at[d - 1],
            {"fs": peer // tp, "tp": peer % tp},
        )

    locals_ = [
        pltpu.make_async_copy(win_ref, w_rows(me), local_sem.at[0]),
        pltpu.make_async_copy(low_ref, l_buf.at[me], local_sem.at[1]),
        pltpu.make_async_copy(wout_ref, o_buf.at[me], local_sem.at[2]),
        pltpu.make_async_copy(tok_ref, tok_rows(mine), local_sem.at[3]),
    ]

    def sends(k):
        @pl.when((me - k >= 0) & (me + 1 < sp))
        def _():
            l_copy(me - k, 0, k == 0).start()
            w_copy(me - k, 0, k == 0).start()

        @pl.when((me + k < sp) & (me >= 1))
        def _():
            l_copy(me + k, 1, k == 0).start()
            w_copy(me + k, 1, k == 0).start()

        @pl.when((me == k) & (me + 1 < sp))
        def _():
            o_copy(me, 0, True).start()

        @pl.when((sp - 1 - me == k) & (me >= 1))
        def _():
            o_copy(me, 1, True).start()

    for k in range(sp - 1):
        sends(k)
        if k == 0:
            for d in range(1, plane):
                tok_copy(d, lax.rem(mine + d, plane), mine).start()
            for copy in locals_:
                copy.start()

        @pl.when(me - 1 - k >= 0)
        def _():
            l_copy(me - 1 - k, 0, False).wait_recv()
            w_copy(me - 1 - k, 0, False).wait_recv()

        @pl.when(me + 1 + k < sp)
        def _():
            l_copy(me + 1 + k, 1, False).wait_recv()
            w_copy(me + 1 + k, 1, False).wait_recv()

    inner = (me >= 1) & (me + 1 < sp)
    for k in range(1, sp - 1):
        @pl.when(inner & (me - k >= 0))
        def _():
            o_copy(me - k, 0, False).wait_recv()
            o_copy(me - k, 0, False).start()

        @pl.when(inner & (me + k < sp))
        def _():
            o_copy(me + k, 1, False).wait_recv()
            o_copy(me + k, 1, False).start()

    for copy in locals_:
        copy.wait()
    for d in range(1, plane):
        tok_copy(d, mine, lax.rem(mine + plane - d, plane)).wait_recv()

    cols = [VALUE_DIM, 2 * HEAD_DIM, KEY_DIM, KEY_DIM, HEAD_DIM, HEAD_DIM]
    starts = [sum(cols[:i]) for i in range(len(cols))]

    def project(b, _):
        x = x_buf[pl.ds(pl.multiple_of(b * rows, rows), rows)].astype(F32)
        normed = rms_rows(x, ngain_ref[...]).astype(BF)
        p = nn(normed, w_buf[...]).astype(BF)
        proj[b, :, : p.shape[1]] = p
        edge_out[b] = p[rows - WINDOW :, starts[4] : starts[4] + 2 * HEAD_DIM]
        low = nt(normed[:, :kc], l_buf[0])
        for s in range(1, sp):
            low += nt(normed[:, s * kc : (s + 1) * kc], l_buf[s])
        proj[b, :, p.shape[1] : p.shape[1] + low.shape[1]] = low.astype(BF)
        return 0

    lax.fori_loop(0, fs, project, 0)
    edge = remote(edge_out, edge_in, edge_sem.at[0], edge_sem.at[1], {"sp": me + 1})

    @pl.when(me + 1 < sp)
    def _():
        edge.start()

    @pl.when(me == 0)
    def _():
        edge_in[...] = jnp.zeros_like(edge_in)

    nb = rows // SPAN
    low_at = sum(cols)
    lower = (
        lax.broadcasted_iota(jnp.int32, (SPAN, SPAN), 0)
        >= lax.broadcasted_iota(jnp.int32, (SPAN, SPAN), 1)
    )
    tri = lower.astype(F32)
    for b in range(fs):
        low = proj[b, :, low_at : low_at + up_ref.shape[0]]
        z = nn(low, up_ref[...]) + bias_ref[...]
        rate = (jnp.minimum(z, 0.0) - jnp.log1p(jnp.exp(-jnp.abs(z)))) / SOFTMAX_TEMPER
        state = None
        before = jnp.zeros((1, KEY_DIM), F32)
        for n in range(nb):
            r0 = n * SPAN
            within = exact(tri, rate[r0 : r0 + SPAN])
            total = within[SPAN - 1 :]
            v = proj[b, r0 : r0 + SPAN, starts[0] : starts[0] + VALUE_DIM]
            q = proj[b, r0 : r0 + SPAN, starts[2] : starts[2] + KEY_DIM].astype(F32)
            k = proj[b, r0 : r0 + SPAN, starts[3] : starts[3] + KEY_DIM].astype(F32)
            q_dec = q * KEY_DIM**-0.5 * jnp.exp(within)
            k_dec = (k * jnp.exp(-within)).astype(BF)
            k_end = (k * jnp.exp(total - within)).astype(BF)
            scores = jnp.where(lower, nt(q_dec.astype(BF), k_dec), 0.0)
            o = nn(scores.astype(BF), v)
            if state is not None:
                o += nt(q_dec.astype(BF), state.astype(BF))
            local_out[b, r0 : r0 + SPAN] = o
            q_far[b, r0 : r0 + SPAN] = (q_dec * jnp.exp(before)).astype(BF)
            update = tn(v, k_end)
            state = update if state is None else jnp.exp(total) * state + update
            before = before + total
        half = (b % 2) * KEY_DIM
        state_out[b // 2, :VALUE_DIM, half : half + KEY_DIM] = state.astype(BF)
        state_out[b // 2, VALUE_DIM:, half : half + KEY_DIM] = jnp.broadcast_to(
            jnp.exp(before), (16, KEY_DIM)
        ).astype(BF)

    def state_copy(d, sender):
        return remote(
            state_out, state_in.at[sender], state_send.at[d - 1], state_recv.at[sender],
            {"sp": me + d},
        )

    for d in range(1, sp):
        @pl.when(me + d < sp)
        def _():
            state_copy(d, me).start()

    @pl.when(me >= 1)
    def _():
        edge.wait_recv()

    qi = lax.broadcasted_iota(jnp.int32, (WINDOW, 2 * WINDOW), 0)
    ki = lax.broadcasted_iota(jnp.int32, (WINDOW, 2 * WINDOW), 1)
    distance = qi + WINDOW - ki
    inside = (distance >= 0) & (distance < WINDOW)
    heads = sink_ref.shape[1]
    for b in range(fs):
        for w in range(rows // WINDOW):
            r0 = w * WINDOW
            here = proj[b, r0 : r0 + WINDOW, starts[4] : starts[4] + 2 * HEAD_DIM]
            if w == 0:
                past = edge_in[b]
                valid = inside & ((ki >= WINDOW) | (me >= 1))
            else:
                past = proj[b, r0 - WINDOW : r0, starts[4] : starts[4] + 2 * HEAD_DIM]
                valid = inside
            band = jnp.concatenate([past, here], 0)
            bk = band[:, :HEAD_DIM]
            bv = band[:, HEAD_DIM:]
            for h in range(heads):
                q0 = starts[1] + h * HEAD_DIM
                q = proj[b, r0 : r0 + WINDOW, q0 : q0 + HEAD_DIM]
                s = jnp.where(valid, nt(q, bk) * HEAD_DIM**-0.5, -1e30)
                sink = sink_ref[0:1, h : h + 1]
                top = jnp.maximum(jnp.max(s, -1, keepdims=True), sink)
                e = jnp.exp(s - top)
                den = jnp.sum(e, -1, keepdims=True) + jnp.exp(sink - top)
                a = nn((e / den).astype(BF), bv).astype(BF)
                h0 = VALUE_DIM + h * HEAD_DIM
                hidden[b, r0 : r0 + WINDOW, h0 : h0 + HEAD_DIM] = a

    for i in range(sp - 1):
        @pl.when(i < me)
        def _():
            state_copy(1, i).wait_recv()

        @pl.when(i >= me)
        def _():
            state_in[i] = jnp.zeros(state_in.shape[1:], BF)

    for b in range(fs):
        half = (b % 2) * KEY_DIM
        incoming = jnp.zeros((VALUE_DIM, KEY_DIM), F32)
        for i in range(sp - 1):
            got = state_in[i, b // 2, :VALUE_DIM, half : half + KEY_DIM].astype(F32)
            kept = state_in[i, b // 2, VALUE_DIM : VALUE_DIM + 1, half : half + KEY_DIM].astype(F32)
            incoming = jnp.where(i < me, kept * incoming + got, incoming)
        o = local_out[b] + nt(q_far[b], incoming.astype(BF))
        hidden[b, :, :VALUE_DIM] = rms_rows(o, hgain_ref[...]).astype(BF)

    forward = 2 * me < sp
    nc = o_buf.shape[2]

    def chunk(t):
        return lax.rem(jnp.where(forward, me + t, me - t) + sp, sp)

    def half_copy(s):
        return remote(half_out.at[s], half_in.at[s], half_send.at[s], half_recv.at[s], {"tp": 1 - c})

    def piece_copy(s, d, target):
        return remote(
            piece_out.at[s, d - 1], piece_in.at[s, d - 1],
            piece_send.at[s, d - 1], piece_recv.at[s, d - 1], {"fs": target},
        )

    def produce(t):
        s = chunk(t)

        @pl.when(jnp.logical_not(inner) & (t > 0))
        def _():
            o_copy(s, 0, False).wait_recv()

        w = o_buf[s]
        for b in range(fs):
            part = nn(hidden[b], w)
            lo, hi = part[:own], part[own:]
            half_out[s, b] = jnp.where(c == 0, hi, lo).astype(BF)
            half_own[s, b] = jnp.where(c == 0, lo, hi)
        half_copy(s).start()

    def combine(t):
        s = chunk(t)
        half_copy(s).wait_recv()
        for d in range(1, fs):
            to = lax.rem(f + d, fs)
            piece_out[s, d - 1] = (half_own[s, to] + half_in[s, to].astype(F32)).astype(BF)
            piece_copy(s, d, to).start()
        piece_own[s] = half_own[s, f] + half_in[s, f].astype(F32)

    def finish(t):
        s = chunk(t)
        total = piece_own[s]
        for d in range(1, fs):
            piece_copy(s, d, f).wait_recv()
            total += piece_in[s, d - 1].astype(F32)
        out_ref[s] = total.astype(BF)

    produce(0)

    def steady(t, _):
        produce(t)
        combine(t - 1)
        return 0

    lax.fori_loop(1, sp, steady, 0)
    combine(sp - 1)

    def close(t, _):
        finish(t)
        s = chunk(t)
        half_copy(s).wait_send()
        for d in range(1, fs):
            piece_copy(s, d, f).wait_send()
        return 0

    lax.fori_loop(0, sp, close, 0)

    for k in range(sp - 1):
        @pl.when((me - k >= 0) & (me + 1 < sp))
        def _():
            l_copy(me - k, 0, False).wait_send()
            w_copy(me - k, 0, False).wait_send()
            o_copy(me - k, 0, False).wait_send()

        @pl.when((me + k < sp) & (me >= 1))
        def _():
            l_copy(me + k, 1, False).wait_send()
            w_copy(me + k, 1, False).wait_send()
            o_copy(me + k, 1, False).wait_send()

    for d in range(1, plane):
        tok_copy(d, mine, mine).wait_send()

    @pl.when(me + 1 < sp)
    def _():
        edge.wait_send()

    for d in range(1, sp):
        @pl.when(me + d < sp)
        def _():
            state_copy(d, me).wait_send()


def per_device(
    tokens,
    norm_gain,
    gla_query_weight,
    gla_key_weight,
    gla_value_weight,
    decay_down,
    decay_up,
    decay_bias,
    head_gain,
    window_query_weight,
    window_key_weight,
    window_value_weight,
    sink_logit,
    gla_output_weight,
    window_output_weight,
):
    fs, tp, sp = (lax.axis_size(n) for n in ("fs", "tp", "sp"))
    heads = sink_logit.shape[0] // fs
    w_in = jnp.concatenate(
        [
            quarter(gla_value_weight, 1),
            quarter(window_query_weight, 1),
            quarter(gla_query_weight, 1),
            quarter(gla_key_weight, 1),
            shared(window_key_weight, heads),
            shared(window_value_weight, heads),
        ],
        1,
    )
    low = decay_down.T
    w_out = jnp.concatenate([quarter(gla_output_weight, 0), quarter(window_output_weight, 0)], 0)
    own = tokens.shape[1]
    rows = own * tp
    kc, width = w_in.shape
    rank = low.shape[0]
    depth, nc = w_out.shape
    vm = pltpu.VMEM
    dma = pltpu.SemaphoreType.DMA
    scratch = [
        vm((fs * rows, tokens.shape[2]), BF),
        vm((sp * kc, width), BF),
        vm((sp, rank, kc), BF),
        vm((sp, depth, nc), BF),
        vm((fs, rows, width + 128), BF),
        vm((fs, WINDOW, 2 * HEAD_DIM), BF),
        vm((fs, WINDOW, 2 * HEAD_DIM), BF),
        vm((fs // 2, VALUE_DIM + 16, 2 * KEY_DIM), BF),
        vm((sp, fs // 2, VALUE_DIM + 16, 2 * KEY_DIM), BF),
        vm((fs, rows, VALUE_DIM), F32),
        vm((fs, rows, KEY_DIM), BF),
        vm((fs, rows, depth), BF),
        vm((sp, fs, own, nc), BF),
        vm((sp, fs, own, nc), BF),
        vm((sp, fs, own, nc), F32),
        vm((sp, fs - 1, own, nc), BF),
        vm((sp, fs - 1, own, nc), BF),
        vm((sp, own, nc), F32),
        dma((4,)),
        dma((fs * tp - 1,)),
        dma((fs * tp - 1,)),
        dma((2, sp)),
        dma((sp,)),
        dma((2, sp)),
        dma((sp,)),
        dma((2, sp)),
        dma((sp,)),
        dma((2,)),
        dma((sp,)),
        dma((sp,)),
        dma((sp,)),
        dma((sp,)),
        dma((sp, fs - 1)),
        dma((sp, fs - 1)),
    ]
    spec = pl.BlockSpec(memory_space=pltpu.VMEM)
    mixed = pl.pallas_call(
        functools.partial(mixer_kernel, (sp, fs, tp)),
        out_shape=jax.ShapeDtypeStruct((sp, own, nc), BF),
        in_specs=[spec] * 9,
        out_specs=spec,
        scratch_shapes=scratch,
        compiler_params=pltpu.CompilerParams(
            has_side_effects=True, vmem_limit_bytes=60 * 1024 * 1024
        ),
    )(
        tokens[0],
        w_in,
        low,
        w_out,
        norm_gain[None],
        quarter(decay_up, 1),
        quarter(decay_bias, 0)[None],
        head_gain[None],
        quarter(sink_logit, 0)[None],
    )
    return mixed.transpose(1, 0, 2).reshape(1, own, sp * nc)


def solution(mesh):
    in_specs = (
        P("fs", ("sp", "tp"), None),
        P(),
        P("sp", "tp"),
        P("sp", "tp"),
        P("sp", "tp"),
        P("sp", None),
        P(None, "tp"),
        P("tp"),
        P(),
        P("sp", "tp"),
        P("sp", "tp"),
        P("sp", "tp"),
        P("tp"),
        P("tp", "sp"),
        P("tp", "sp"),
    )
    out_specs = P("fs", ("sp", "tp"), None)
    return jax.shard_map(
        per_device, mesh=mesh, in_specs=in_specs, out_specs=out_specs, check_vma=False
    )
```

```python
import functools

import jax
import jax.numpy as jnp
from jax import lax
from jax.experimental import pallas as pl
from jax.experimental.pallas import tpu as pltpu
from jax.sharding import PartitionSpec as P

KEY_DIM = 64
VALUE_DIM = 128
SWA_HEADS = 16
KV_HEADS = 4
HEAD_DIM = 64
WINDOW = 128
SPAN = 64

EPS = 1e-06
SOFTMAX_TEMPER = 16.0
BF = jnp.bfloat16
F32 = jnp.float32


def rms_rows(values, gain):
    mean_square = jnp.mean(values * values, axis=-1, keepdims=True)
    return values * lax.rsqrt(mean_square + EPS) * gain


def nt(a, b):
    return lax.dot_general(a, b, (((1,), (1,)), ((), ())), preferred_element_type=F32)


def nn(a, b):
    return lax.dot_general(a, b, (((1,), (0,)), ((), ())), preferred_element_type=F32)


def tn(a, b):
    return lax.dot_general(a, b, (((0,), (0,)), ((), ())), preferred_element_type=F32)


def exact(a, b):
    return lax.dot_general(
        a, b, (((1,), (0,)), ((), ())), precision=lax.Precision.HIGHEST, preferred_element_type=F32
    )


def mixer_kernel(
    sizes,
    tok_ref,
    gv_ref,
    wq_ref,
    gq_ref,
    gk_ref,
    wk_ref,
    wv_ref,
    low_ref,
    go_ref,
    wo_ref,
    ngain_ref,
    up_ref,
    bias_ref,
    hgain_ref,
    sink_ref,
    out_ref,
    x_buf,
    w_buf,
    l_buf,
    o_buf,
    proj,
    edge_out,
    edge_in,
    state_out,
    state_in,
    local_out,
    q_far,
    hidden,
    half_out,
    half_in,
    half_own,
    piece_out,
    piece_in,
    piece_own,
    local_sem,
    tok_send,
    tok_recv,
    w_send,
    w_recv,
    l_send,
    l_recv,
    v_send,
    v_recv,
    vp_send,
    vp_recv,
    lp_send,
    lp_recv,
    o_send,
    o_recv,
    edge_sem,
    state_send,
    state_recv,
    half_send,
    half_recv,
    piece_send,
    piece_recv,
):
    sp, fs, tp = sizes
    me = lax.axis_index("sp")
    f = lax.axis_index("fs")
    c = lax.axis_index("tp")
    plane = fs * tp
    mine = f * tp + c
    own = tok_ref.shape[0]
    rows = own * tp
    kc = gv_ref.shape[0]
    MESH = pl.DeviceIdType.MESH

    def remote(src, dst, ssem, rsem, target):
        return pltpu.make_async_remote_copy(
            src_ref=src, dst_ref=dst, send_sem=ssem, recv_sem=rsem,
            device_id=target, device_id_type=MESH,
        )

    def w_rows(s):
        return w_buf.at[pl.ds(pl.multiple_of(s * kc, kc), kc)]

    def w_copy(s, way, first):
        target = {"sp": me + (1 if way == 0 else -1)}
        return remote(
            w_main(s), w_main(s), w_send.at[way, s], w_recv.at[s], target
        )

    side = f % 2
    part = kc // 2
    lpart = low_ref.shape[0] // 2

    def w_main(s):
        return w_rows(s).at[:, : starts[4]]

    def v_rows(s, h):
        at = pl.multiple_of(s * kc + h * part, part)
        return w_buf.at[pl.ds(at, part), starts[4] : starts[4] + 2 * HEAD_DIM]

    def l_rows(s, h):
        return l_buf.at[s, pl.ds(pl.multiple_of(h * lpart, lpart), lpart)]

    def v_copy(s, way):
        target = {"sp": me + (1 if way == 0 else -1)}
        return remote(v_rows(s, side), v_rows(s, side), v_send.at[way, s], v_recv.at[s], target)

    def lh_copy(s, way):
        target = {"sp": me + (1 if way == 0 else -1)}
        return remote(l_rows(s, side), l_rows(s, side), l_send.at[way, s], l_recv.at[s], target)

    def pair_copies(s, h):
        target = {"fs": f + 1 - 2 * side}
        return (
            remote(v_rows(s, h), v_rows(s, h), vp_send.at[s], vp_recv.at[s], target),
            remote(l_rows(s, h), l_rows(s, h), lp_send.at[s], lp_recv.at[s], target),
        )

    class l_copy:
        def __init__(self, s, way, first):
            self.s = s
            self.both = (v_copy(s, way), lh_copy(s, way))

        def start(self):
            for copy in self.both:
                copy.start()

        def wait_recv(self):
            for copy, onward in zip(self.both, pair_copies(self.s, side)):
                copy.wait_recv()
                onward.start()

        def wait_send(self):
            for copy in self.both:
                copy.wait_send()

    def o_copy(s, way, first):
        target = {"sp": me + (1 if way == 0 else -1)}
        return remote(
            o_buf.at[s], o_buf.at[s], o_send.at[way, s], o_recv.at[s], target
        )

    def tok_rows(i):
        return x_buf.at[pl.ds(pl.multiple_of(i * own, own), own)]

    def tok_copy(d, peer, sender):
        return remote(
            tok_ref, tok_rows(sender), tok_send.at[d - 1], tok_recv.at[d - 1],
            {"fs": peer // tp, "tp": peer % tp},
        )

    def pick(ref, width, which):
        value = ref[:, :width]
        for i in range(1, ref.shape[1] // width):
            value = jnp.where(which == i, ref[:, i * width : (i + 1) * width], value)
        return value

    def lanes(ref, width):
        return ref.at[:, pl.ds(pl.multiple_of(f * width, width), width)]

    def depth(ref, width):
        return ref.at[pl.ds(pl.multiple_of(f * width, width), width)]

    cols = [VALUE_DIM, 2 * HEAD_DIM, KEY_DIM, KEY_DIM, HEAD_DIM, HEAD_DIM]
    starts = [sum(cols[:i]) for i in range(len(cols))]
    gd = go_ref.shape[0] // fs
    wd = wo_ref.shape[0] // fs
    heads = sink_ref.shape[1] // fs
    copies_in = [
        (lanes(gv_ref, cols[0]), w_rows(me).at[:, : cols[0]]),
        (lanes(wq_ref, cols[1]), w_rows(me).at[:, starts[1] : starts[2]]),
        (depth(go_ref, gd), o_buf.at[me, pl.ds(0, gd)]),
        (depth(wo_ref, wd), o_buf.at[me, pl.ds(gd, wd)]),
        (low_ref, l_buf.at[me]),
        (tok_ref, tok_rows(mine)),
    ]
    locals_ = [
        pltpu.make_async_copy(a, b, local_sem.at[i]) for i, (a, b) in enumerate(copies_in)
    ]
    for copy in locals_:
        copy.start()
    for d in range(1, plane):
        tok_copy(d, lax.rem(mine + d, plane), mine).start()
    own_rows = pl.ds(pl.multiple_of(me * kc, kc), kc)
    kv = (f * heads) // (SWA_HEADS // KV_HEADS)
    w_buf[own_rows, starts[2] : starts[4]] = jnp.concatenate(
        [pick(gq_ref, KEY_DIM, f), pick(gk_ref, KEY_DIM, f)], 1
    )
    w_buf[own_rows, starts[4] :] = jnp.concatenate(
        [pick(wk_ref, HEAD_DIM, kv), pick(wv_ref, HEAD_DIM, kv)], 1
    )
    for copy in locals_[:5]:
        copy.wait()

    def sends(k):
        @pl.when((me - k >= 0) & (me + 1 < sp))
        def _():
            l_copy(me - k, 0, k == 0).start()
            w_copy(me - k, 0, k == 0).start()

        @pl.when((me + k < sp) & (me >= 1))
        def _():
            l_copy(me + k, 1, k == 0).start()
            w_copy(me + k, 1, k == 0).start()

        @pl.when((me == k) & (me + 1 < sp))
        def _():
            o_copy(me, 0, True).start()

        @pl.when((sp - 1 - me == k) & (me >= 1))
        def _():
            o_copy(me, 1, True).start()

    for k in range(sp - 1):
        sends(k)

        @pl.when(me - 1 - k >= 0)
        def _():
            l_copy(me - 1 - k, 0, False).wait_recv()
            w_copy(me - 1 - k, 0, False).wait_recv()

        @pl.when(me + 1 + k < sp)
        def _():
            l_copy(me + 1 + k, 1, False).wait_recv()
            w_copy(me + 1 + k, 1, False).wait_recv()

    inner = (me >= 1) & (me + 1 < sp)
    for k in range(1, sp - 1):
        @pl.when(inner & (me - k >= 0))
        def _():
            o_copy(me - k, 0, False).wait_recv()
            o_copy(me - k, 0, False).start()

        @pl.when(inner & (me + k < sp))
        def _():
            o_copy(me + k, 1, False).wait_recv()
            o_copy(me + k, 1, False).start()

    for copy in locals_[5:]:
        copy.wait()
    for i in range(sp):
        @pl.when(i != me)
        def _():
            for copy in pair_copies(i, 1 - side):
                copy.wait_recv()

    for d in range(1, plane):
        tok_copy(d, mine, lax.rem(mine + plane - d, plane)).wait_recv()


    def project(b, _):
        x = x_buf[pl.ds(pl.multiple_of(b * rows, rows), rows)].astype(F32)
        normed = rms_rows(x, ngain_ref[...]).astype(BF)
        p = nn(normed, w_buf[...]).astype(BF)
        proj[b, :, : p.shape[1]] = p
        edge_out[b] = p[rows - WINDOW :, starts[4] : starts[4] + 2 * HEAD_DIM]
        low = nt(normed[:, :kc], l_buf[0])
        for s in range(1, sp):
            low += nt(normed[:, s * kc : (s + 1) * kc], l_buf[s])
        proj[b, :, p.shape[1] : p.shape[1] + low.shape[1]] = low.astype(BF)
        return 0

    lax.fori_loop(0, fs, project, 0)
    edge = remote(edge_out, edge_in, edge_sem.at[0], edge_sem.at[1], {"sp": me + 1})

    @pl.when(me + 1 < sp)
    def _():
        edge.start()

    @pl.when(me == 0)
    def _():
        edge_in[...] = jnp.zeros_like(edge_in)

    nb = rows // SPAN
    low_at = sum(cols)
    lower = (
        lax.broadcasted_iota(jnp.int32, (SPAN, SPAN), 0)
        >= lax.broadcasted_iota(jnp.int32, (SPAN, SPAN), 1)
    )
    tri = lower.astype(F32)
    up = pick(up_ref, KEY_DIM, f)
    bias = pick(bias_ref, KEY_DIM, f)
    sinks = pick(sink_ref, heads, f)
    for b in range(fs):
        low = proj[b, :, low_at : low_at + up_ref.shape[0]]
        z = nn(low, up) + bias
        rate = (jnp.minimum(z, 0.0) - jnp.log1p(jnp.exp(-jnp.abs(z)))) / SOFTMAX_TEMPER
        state = None
        before = jnp.zeros((1, KEY_DIM), F32)
        for n in range(nb):
            r0 = n * SPAN
            within = exact(tri, rate[r0 : r0 + SPAN])
            total = within[SPAN - 1 :]
            v = proj[b, r0 : r0 + SPAN, starts[0] : starts[0] + VALUE_DIM]
            q = proj[b, r0 : r0 + SPAN, starts[2] : starts[2] + KEY_DIM].astype(F32)
            k = proj[b, r0 : r0 + SPAN, starts[3] : starts[3] + KEY_DIM].astype(F32)
            q_dec = q * KEY_DIM**-0.5 * jnp.exp(within)
            k_dec = (k * jnp.exp(-within)).astype(BF)
            k_end = (k * jnp.exp(total - within)).astype(BF)
            scores = jnp.where(lower, nt(q_dec.astype(BF), k_dec), 0.0)
            o = nn(scores.astype(BF), v)
            if state is not None:
                o += nt(q_dec.astype(BF), state.astype(BF))
            local_out[b, r0 : r0 + SPAN] = o
            q_far[b, r0 : r0 + SPAN] = (q_dec * jnp.exp(before)).astype(BF)
            update = tn(v, k_end)
            state = update if state is None else jnp.exp(total) * state + update
            before = before + total
        half = (b % 2) * KEY_DIM
        state_out[b // 2, :VALUE_DIM, half : half + KEY_DIM] = state.astype(BF)
        state_out[b // 2, VALUE_DIM:, half : half + KEY_DIM] = jnp.broadcast_to(
            jnp.exp(before), (16, KEY_DIM)
        ).astype(BF)

    def state_copy(d, sender):
        return remote(
            state_out, state_in.at[sender], state_send.at[d - 1], state_recv.at[sender],
            {"sp": me + d},
        )

    for d in range(1, sp):
        @pl.when(me + d < sp)
        def _():
            state_copy(d, me).start()

    @pl.when(me >= 1)
    def _():
        edge.wait_recv()

    qi = lax.broadcasted_iota(jnp.int32, (WINDOW, 2 * WINDOW), 0)
    ki = lax.broadcasted_iota(jnp.int32, (WINDOW, 2 * WINDOW), 1)
    distance = qi + WINDOW - ki
    inside = (distance >= 0) & (distance < WINDOW)
    for b in range(fs):
        for w in range(rows // WINDOW):
            r0 = w * WINDOW
            here = proj[b, r0 : r0 + WINDOW, starts[4] : starts[4] + 2 * HEAD_DIM]
            if w == 0:
                past = edge_in[b]
                valid = inside & ((ki >= WINDOW) | (me >= 1))
            else:
                past = proj[b, r0 - WINDOW : r0, starts[4] : starts[4] + 2 * HEAD_DIM]
                valid = inside
            band = jnp.concatenate([past, here], 0)
            bk = band[:, :HEAD_DIM]
            bv = band[:, HEAD_DIM:]
            for h in range(heads):
                q0 = starts[1] + h * HEAD_DIM
                q = proj[b, r0 : r0 + WINDOW, q0 : q0 + HEAD_DIM]
                s = jnp.where(valid, nt(q, bk) * HEAD_DIM**-0.5, -1e30)
                sink = sinks[:, h : h + 1]
                top = jnp.maximum(jnp.max(s, -1, keepdims=True), sink)
                e = jnp.exp(s - top)
                den = jnp.sum(e, -1, keepdims=True) + jnp.exp(sink - top)
                a = nn((e / den).astype(BF), bv).astype(BF)
                h0 = VALUE_DIM + h * HEAD_DIM
                hidden[b, r0 : r0 + WINDOW, h0 : h0 + HEAD_DIM] = a

    for i in range(sp - 1):
        @pl.when(i < me)
        def _():
            state_copy(1, i).wait_recv()

        @pl.when(i >= me)
        def _():
            state_in[i] = jnp.zeros(state_in.shape[1:], BF)

    for b in range(fs):
        half = (b % 2) * KEY_DIM
        incoming = jnp.zeros((VALUE_DIM, KEY_DIM), F32)
        for i in range(sp - 1):
            got = state_in[i, b // 2, :VALUE_DIM, half : half + KEY_DIM].astype(F32)
            kept = state_in[i, b // 2, VALUE_DIM : VALUE_DIM + 1, half : half + KEY_DIM].astype(F32)
            incoming = jnp.where(i < me, kept * incoming + got, incoming)
        o = local_out[b] + nt(q_far[b], incoming.astype(BF))
        hidden[b, :, :VALUE_DIM] = rms_rows(o, hgain_ref[...]).astype(BF)

    forward = 2 * me < sp
    nc = o_buf.shape[2]

    def chunk(t):
        return lax.rem(jnp.where(forward, me + t, me - t) + sp, sp)

    def half_copy(s):
        return remote(half_out.at[s], half_in.at[s], half_send.at[s], half_recv.at[s], {"tp": 1 - c})

    def piece_copy(s, d, target):
        return remote(
            piece_out.at[s, d - 1], piece_in.at[s, d - 1],
            piece_send.at[s, d - 1], piece_recv.at[s, d - 1], {"fs": target},
        )

    def produce(t):
        s = chunk(t)

        @pl.when(jnp.logical_not(inner) & (t > 0))
        def _():
            o_copy(s, 0, False).wait_recv()

        w = o_buf[s]
        for b in range(fs):
            part = nn(hidden[b], w)
            lo, hi = part[:own], part[own:]
            half_out[s, b] = jnp.where(c == 0, hi, lo).astype(BF)
            half_own[s, b] = jnp.where(c == 0, lo, hi)
        half_copy(s).start()

    def combine(t):
        s = chunk(t)
        half_copy(s).wait_recv()
        for d in range(1, fs):
            to = lax.rem(f + d, fs)
            piece_out[s, d - 1] = (half_own[s, to] + half_in[s, to].astype(F32)).astype(BF)
            piece_copy(s, d, to).start()
        piece_own[s] = half_own[s, f] + half_in[s, f].astype(F32)

    def finish(t):
        s = chunk(t)
        total = piece_own[s]
        for d in range(1, fs):
            piece_copy(s, d, f).wait_recv()
            total += piece_in[s, d - 1].astype(F32)
        out_ref[s] = total.astype(BF)

    produce(0)

    def steady(t, _):
        produce(t)
        combine(t - 1)
        return 0

    lax.fori_loop(1, sp, steady, 0)
    combine(sp - 1)

    def close(t, _):
        finish(t)
        s = chunk(t)
        half_copy(s).wait_send()
        for d in range(1, fs):
            piece_copy(s, d, f).wait_send()
        return 0

    lax.fori_loop(0, sp, close, 0)

    for k in range(sp - 1):
        @pl.when((me - k >= 0) & (me + 1 < sp))
        def _():
            l_copy(me - k, 0, False).wait_send()
            w_copy(me - k, 0, False).wait_send()
            o_copy(me - k, 0, False).wait_send()

        @pl.when((me + k < sp) & (me >= 1))
        def _():
            l_copy(me + k, 1, False).wait_send()
            w_copy(me + k, 1, False).wait_send()
            o_copy(me + k, 1, False).wait_send()

    for i in range(sp):
        @pl.when(i != me)
        def _():
            for copy in pair_copies(i, side):
                copy.wait_send()

    for d in range(1, plane):
        tok_copy(d, mine, mine).wait_send()

    @pl.when(me + 1 < sp)
    def _():
        edge.wait_send()

    for d in range(1, sp):
        @pl.when(me + d < sp)
        def _():
            state_copy(d, me).wait_send()


def per_device(
    tokens,
    norm_gain,
    gla_query_weight,
    gla_key_weight,
    gla_value_weight,
    decay_down,
    decay_up,
    decay_bias,
    head_gain,
    window_query_weight,
    window_key_weight,
    window_value_weight,
    sink_logit,
    gla_output_weight,
    window_output_weight,
):
    fs, tp, sp = (lax.axis_size(n) for n in ("fs", "tp", "sp"))
    low = decay_down.T
    own = tokens.shape[1]
    rows = own * tp
    kc = decay_down.shape[0]
    width = VALUE_DIM + 4 * HEAD_DIM + 2 * KEY_DIM
    rank = low.shape[0]
    depth = (gla_output_weight.shape[0] + window_output_weight.shape[0]) // fs
    nc = gla_output_weight.shape[1]
    vm = pltpu.VMEM
    dma = pltpu.SemaphoreType.DMA
    scratch = [
        vm((fs * rows, tokens.shape[2]), BF),
        vm((sp * kc, width), BF),
        vm((sp, rank, kc), BF),
        vm((sp, depth, nc), BF),
        vm((fs, rows, width + 128), BF),
        vm((fs, WINDOW, 2 * HEAD_DIM), BF),
        vm((fs, WINDOW, 2 * HEAD_DIM), BF),
        vm((fs // 2, VALUE_DIM + 16, 2 * KEY_DIM), BF),
        vm((sp, fs // 2, VALUE_DIM + 16, 2 * KEY_DIM), BF),
        vm((fs, rows, VALUE_DIM), F32),
        vm((fs, rows, KEY_DIM), BF),
        vm((fs, rows, depth), BF),
        vm((sp, fs, own, nc), BF),
        vm((sp, fs, own, nc), BF),
        vm((sp, fs, own, nc), F32),
        vm((sp, fs - 1, own, nc), BF),
        vm((sp, fs - 1, own, nc), BF),
        vm((sp, own, nc), F32),
        dma((6,)),
        dma((fs * tp - 1,)),
        dma((fs * tp - 1,)),
        dma((2, sp)),
        dma((sp,)),
        dma((2, sp)),
        dma((sp,)),
        dma((2, sp)),
        dma((sp,)),
        dma((sp,)),
        dma((sp,)),
        dma((sp,)),
        dma((sp,)),
        dma((2, sp)),
        dma((sp,)),
        dma((2,)),
        dma((sp,)),
        dma((sp,)),
        dma((sp,)),
        dma((sp,)),
        dma((sp, fs - 1)),
        dma((sp, fs - 1)),
    ]
    spec = pl.BlockSpec(memory_space=pltpu.VMEM)
    anywhere = pl.BlockSpec(memory_space=pl.ANY)
    mixed = pl.pallas_call(
        functools.partial(mixer_kernel, (sp, fs, tp)),
        out_shape=jax.ShapeDtypeStruct((sp, own, nc), BF),
        in_specs=[
            anywhere if i in (1, 2, 8, 9) else spec for i in range(15)
        ],
        out_specs=spec,
        scratch_shapes=scratch,
        compiler_params=pltpu.CompilerParams(
            has_side_effects=True, vmem_limit_bytes=60 * 1024 * 1024
        ),
    )(
        tokens[0],
        gla_value_weight,
        window_query_weight,
        gla_query_weight,
        gla_key_weight,
        window_key_weight,
        window_value_weight,
        low,
        gla_output_weight,
        window_output_weight,
        norm_gain[None],
        decay_up,
        decay_bias[None],
        head_gain[None],
        sink_logit[None],
    )
    return mixed.transpose(1, 0, 2).reshape(1, own, sp * nc)


def solution(mesh):
    in_specs = (
        P("fs", ("sp", "tp"), None),
        P(),
        P("sp", "tp"),
        P("sp", "tp"),
        P("sp", "tp"),
        P("sp", None),
        P(None, "tp"),
        P("tp"),
        P(),
        P("sp", "tp"),
        P("sp", "tp"),
        P("sp", "tp"),
        P("tp"),
        P("tp", "sp"),
        P("tp", "sp"),
    )
    out_specs = P("fs", ("sp", "tp"), None)
    return jax.shard_map(
        per_device, mesh=mesh, in_specs=in_specs, out_specs=out_specs, check_vma=False
    )
```

```python
import functools

import jax
import jax.numpy as jnp
from jax import lax
from jax.experimental import pallas as pl
from jax.experimental.pallas import tpu as pltpu
from jax.sharding import PartitionSpec as P

KEY_DIM = 64
VALUE_DIM = 128
SWA_HEADS = 16
KV_HEADS = 4
HEAD_DIM = 64
WINDOW = 128
SPAN = 64

EPS = 1e-06
SOFTMAX_TEMPER = 16.0
BF = jnp.bfloat16
F32 = jnp.float32


def rms_rows(values, gain):
    mean_square = jnp.mean(values * values, axis=-1, keepdims=True)
    return values * lax.rsqrt(mean_square + EPS) * gain


def nt(a, b):
    return lax.dot_general(a, b, (((1,), (1,)), ((), ())), preferred_element_type=F32)


def nn(a, b):
    return lax.dot_general(a, b, (((1,), (0,)), ((), ())), preferred_element_type=F32)


def tn(a, b):
    return lax.dot_general(a, b, (((0,), (0,)), ((), ())), preferred_element_type=F32)


def exact(a, b):
    return lax.dot_general(
        a, b, (((1,), (0,)), ((), ())), precision=lax.Precision.HIGHEST, preferred_element_type=F32
    )


def mixer_kernel(
    sizes,
    tok_ref,
    gv_ref,
    wq_ref,
    gq_ref,
    gk_ref,
    wk_ref,
    wv_ref,
    low_ref,
    go_ref,
    wo_ref,
    ngain_ref,
    up_ref,
    bias_ref,
    hgain_ref,
    sink_ref,
    out_ref,
    x_buf,
    w_buf,
    l_buf,
    o_buf,
    proj,
    edge_out,
    edge_in,
    state_out,
    state_in,
    local_out,
    q_far,
    hidden,
    half_out,
    half_in,
    half_own,
    piece_out,
    piece_in,
    piece_own,
    local_sem,
    tok_send,
    tok_recv,
    w_send,
    w_recv,
    l_send,
    l_recv,
    v_send,
    v_recv,
    vp_send,
    vp_recv,
    lp_send,
    lp_recv,
    o_send,
    o_recv,
    edge_sem,
    state_send,
    state_recv,
    half_send,
    half_recv,
    piece_send,
    piece_recv,
):
    sp, fs, tp = sizes
    me = lax.axis_index("sp")
    f = lax.axis_index("fs")
    c = lax.axis_index("tp")
    plane = fs * tp
    mine = f * tp + c
    own = tok_ref.shape[0]
    rows = own * tp
    kc = gv_ref.shape[0]
    MESH = pl.DeviceIdType.MESH

    def remote(src, dst, ssem, rsem, target):
        return pltpu.make_async_remote_copy(
            src_ref=src, dst_ref=dst, send_sem=ssem, recv_sem=rsem,
            device_id=target, device_id_type=MESH,
        )

    def w_rows(s):
        return w_buf.at[pl.ds(pl.multiple_of(s * kc, kc), kc)]

    def w_copy(s, way, first):
        target = {"sp": me + (1 if way == 0 else -1)}
        return remote(
            w_main(s), w_main(s), w_send.at[way, s], w_recv.at[s], target
        )

    side = f % 2
    part = kc // 2
    lpart = low_ref.shape[0] // 2

    def w_main(s):
        return w_rows(s).at[:, : starts[4]]

    def v_rows(s, h):
        at = pl.multiple_of(s * kc + h * part, part)
        return w_buf.at[pl.ds(at, part), starts[4] : starts[4] + 2 * HEAD_DIM]

    def l_rows(s, h):
        return l_buf.at[s, pl.ds(pl.multiple_of(h * lpart, lpart), lpart)]

    def v_copy(s, way):
        target = {"sp": me + (1 if way == 0 else -1)}
        return remote(v_rows(s, side), v_rows(s, side), v_send.at[way, s], v_recv.at[s], target)

    def lh_copy(s, way):
        target = {"sp": me + (1 if way == 0 else -1)}
        return remote(l_rows(s, side), l_rows(s, side), l_send.at[way, s], l_recv.at[s], target)

    def pair_copies(s, h):
        target = {"fs": f + 1 - 2 * side}
        return (
            remote(v_rows(s, h), v_rows(s, h), vp_send.at[s], vp_recv.at[s], target),
            remote(l_rows(s, h), l_rows(s, h), lp_send.at[s], lp_recv.at[s], target),
        )

    class l_copy:
        def __init__(self, s, way, first):
            self.s = s
            self.both = (v_copy(s, way), lh_copy(s, way))

        def start(self):
            for copy in self.both:
                copy.start()

        def wait_recv(self):
            for copy, onward in zip(self.both, pair_copies(self.s, side)):
                copy.wait_recv()
                onward.start()

        def wait_send(self):
            for copy in self.both:
                copy.wait_send()

    def o_copy(s, way, first):
        target = {"sp": me + (1 if way == 0 else -1)}
        return remote(
            o_buf.at[s], o_buf.at[s], o_send.at[way, s], o_recv.at[s], target
        )

    def tok_rows(i):
        return x_buf.at[pl.ds(pl.multiple_of(i * own, own), own)]

    def tok_copy(d, peer, sender):
        return remote(
            tok_ref, tok_rows(sender), tok_send.at[d - 1], tok_recv.at[d - 1],
            {"fs": peer // tp, "tp": peer % tp},
        )

    def pick(ref, width, which):
        value = ref[:, :width]
        for i in range(1, ref.shape[1] // width):
            value = jnp.where(which == i, ref[:, i * width : (i + 1) * width], value)
        return value

    def lanes(ref, width):
        return ref.at[:, pl.ds(pl.multiple_of(f * width, width), width)]

    def depth(ref, width):
        return ref.at[pl.ds(pl.multiple_of(f * width, width), width)]

    cols = [VALUE_DIM, 2 * HEAD_DIM, KEY_DIM, KEY_DIM, HEAD_DIM, HEAD_DIM]
    starts = [sum(cols[:i]) for i in range(len(cols))]
    gd = go_ref.shape[0] // fs
    wd = wo_ref.shape[0] // fs
    heads = sink_ref.shape[1] // fs
    copies_in = [
        (lanes(gv_ref, cols[0]), w_rows(me).at[:, : cols[0]]),
        (lanes(wq_ref, cols[1]), w_rows(me).at[:, starts[1] : starts[2]]),
        (depth(go_ref, gd), o_buf.at[me, pl.ds(0, gd)]),
        (depth(wo_ref, wd), o_buf.at[me, pl.ds(gd, wd)]),
        (low_ref, l_buf.at[me]),
        (tok_ref, tok_rows(mine)),
    ]
    locals_ = [
        pltpu.make_async_copy(a, b, local_sem.at[i]) for i, (a, b) in enumerate(copies_in)
    ]
    for copy in locals_:
        copy.start()
    for d in range(1, plane):
        tok_copy(d, lax.rem(mine + d, plane), mine).start()
    own_rows = pl.ds(pl.multiple_of(me * kc, kc), kc)
    kv = (f * heads) // (SWA_HEADS // KV_HEADS)
    w_buf[own_rows, starts[2] : starts[4]] = jnp.concatenate(
        [pick(gq_ref, KEY_DIM, f), pick(gk_ref, KEY_DIM, f)], 1
    )
    w_buf[own_rows, starts[4] :] = jnp.concatenate(
        [pick(wk_ref, HEAD_DIM, kv), pick(wv_ref, HEAD_DIM, kv)], 1
    )
    for copy in locals_[:5]:
        copy.wait()

    def sends(k):
        @pl.when((me - k >= 0) & (me + 1 < sp))
        def _():
            l_copy(me - k, 0, k == 0).start()
            w_copy(me - k, 0, k == 0).start()

        @pl.when((me + k < sp) & (me >= 1))
        def _():
            l_copy(me + k, 1, k == 0).start()
            w_copy(me + k, 1, k == 0).start()

        @pl.when((me == k) & (me + 1 < sp))
        def _():
            o_copy(me, 0, True).start()

        @pl.when((sp - 1 - me == k) & (me >= 1))
        def _():
            o_copy(me, 1, True).start()

    for k in range(sp - 1):
        sends(k)

        @pl.when(me - 1 - k >= 0)
        def _():
            l_copy(me - 1 - k, 0, False).wait_recv()
            w_copy(me - 1 - k, 0, False).wait_recv()

        @pl.when(me + 1 + k < sp)
        def _():
            l_copy(me + 1 + k, 1, False).wait_recv()
            w_copy(me + 1 + k, 1, False).wait_recv()

    inner = (me >= 1) & (me + 1 < sp)
    for k in range(1, sp - 1):
        @pl.when(inner & (me - k >= 0))
        def _():
            o_copy(me - k, 0, False).wait_recv()
            o_copy(me - k, 0, False).start()

        @pl.when(inner & (me + k < sp))
        def _():
            o_copy(me + k, 1, False).wait_recv()
            o_copy(me + k, 1, False).start()

    for copy in locals_[5:]:
        copy.wait()
    for i in range(sp):
        @pl.when(i != me)
        def _():
            for copy in pair_copies(i, 1 - side):
                copy.wait_recv()

    for d in range(1, plane):
        tok_copy(d, mine, lax.rem(mine + plane - d, plane)).wait_recv()


    def project(b, _):
        x = x_buf[pl.ds(pl.multiple_of(b * rows, rows), rows)].astype(F32)
        normed = rms_rows(x, ngain_ref[...]).astype(BF)
        p = nn(normed, w_buf[...]).astype(BF)
        proj[b, :, : p.shape[1]] = p
        edge_out[b] = p[rows - WINDOW :, starts[4] : starts[4] + 2 * HEAD_DIM]
        low = nt(normed[:, :kc], l_buf[0])
        for s in range(1, sp):
            low += nt(normed[:, s * kc : (s + 1) * kc], l_buf[s])
        proj[b, :, p.shape[1] : p.shape[1] + low.shape[1]] = low.astype(BF)
        return 0

    lax.fori_loop(0, fs, project, 0)
    edge = remote(edge_out, edge_in, edge_sem.at[0], edge_sem.at[1], {"sp": me + 1})

    @pl.when(me + 1 < sp)
    def _():
        edge.start()

    @pl.when(me == 0)
    def _():
        edge_in[...] = jnp.zeros_like(edge_in)

    nb = rows // SPAN
    low_at = sum(cols)
    lower = (
        lax.broadcasted_iota(jnp.int32, (SPAN, SPAN), 0)
        >= lax.broadcasted_iota(jnp.int32, (SPAN, SPAN), 1)
    )
    tri = lower.astype(F32)
    up = pick(up_ref, KEY_DIM, f)
    bias = pick(bias_ref, KEY_DIM, f)
    sinks = pick(sink_ref, heads, f)
    for b in range(fs):
        low = proj[b, :, low_at : low_at + up_ref.shape[0]]
        z = nn(low, up) + bias
        rate = (jnp.minimum(z, 0.0) - jnp.log1p(jnp.exp(-jnp.abs(z)))) / SOFTMAX_TEMPER
        state = None
        before = jnp.zeros((1, KEY_DIM), F32)
        for n in range(nb):
            r0 = n * SPAN
            within = exact(tri, rate[r0 : r0 + SPAN])
            total = within[SPAN - 1 :]
            v = proj[b, r0 : r0 + SPAN, starts[0] : starts[0] + VALUE_DIM]
            q = proj[b, r0 : r0 + SPAN, starts[2] : starts[2] + KEY_DIM].astype(F32)
            k = proj[b, r0 : r0 + SPAN, starts[3] : starts[3] + KEY_DIM].astype(F32)
            q_dec = q * KEY_DIM**-0.5 * jnp.exp(within)
            k_dec = (k * jnp.exp(-within)).astype(BF)
            k_end = (k * jnp.exp(total - within)).astype(BF)
            scores = jnp.where(lower, nt(q_dec.astype(BF), k_dec), 0.0)
            o = nn(scores.astype(BF), v)
            if state is not None:
                o += nt(q_dec.astype(BF), state.astype(BF))
            local_out[b, r0 : r0 + SPAN] = o
            q_far[b, r0 : r0 + SPAN] = (q_dec * jnp.exp(before)).astype(BF)
            update = tn(v, k_end)
            state = update if state is None else jnp.exp(total) * state + update
            before = before + total
        half = (b % 2) * KEY_DIM
        state_out[b // 2, :VALUE_DIM, half : half + KEY_DIM] = state.astype(BF)
        state_out[b // 2, VALUE_DIM:, half : half + KEY_DIM] = jnp.broadcast_to(
            jnp.exp(before), (16, KEY_DIM)
        ).astype(BF)

    def state_copy(d, sender):
        return remote(
            state_out, state_in.at[sender], state_send.at[d - 1], state_recv.at[sender],
            {"sp": me + d},
        )

    for d in range(1, sp):
        @pl.when(me + d < sp)
        def _():
            state_copy(d, me).start()

    @pl.when(me >= 1)
    def _():
        edge.wait_recv()

    qi = lax.broadcasted_iota(jnp.int32, (WINDOW, 2 * WINDOW), 0)
    ki = lax.broadcasted_iota(jnp.int32, (WINDOW, 2 * WINDOW), 1)
    distance = qi + WINDOW - ki
    inside = (distance >= 0) & (distance < WINDOW)
    for b in range(fs):
        for w in range(rows // WINDOW):
            r0 = w * WINDOW
            here = proj[b, r0 : r0 + WINDOW, starts[4] : starts[4] + 2 * HEAD_DIM]
            if w == 0:
                past = edge_in[b]
                valid = inside & ((ki >= WINDOW) | (me >= 1))
            else:
                past = proj[b, r0 - WINDOW : r0, starts[4] : starts[4] + 2 * HEAD_DIM]
                valid = inside
            band = jnp.concatenate([past, here], 0)
            bk = band[:, :HEAD_DIM]
            bv = band[:, HEAD_DIM:]
            for h in range(heads):
                q0 = starts[1] + h * HEAD_DIM
                q = proj[b, r0 : r0 + WINDOW, q0 : q0 + HEAD_DIM]
                s = jnp.where(valid, nt(q, bk) * HEAD_DIM**-0.5, -1e30)
                sink = sinks[:, h : h + 1]
                top = jnp.maximum(jnp.max(s, -1, keepdims=True), sink)
                e = jnp.exp(s - top)
                den = jnp.sum(e, -1, keepdims=True) + jnp.exp(sink - top)
                a = nn((e / den).astype(BF), bv).astype(BF)
                h0 = VALUE_DIM + h * HEAD_DIM
                hidden[b, r0 : r0 + WINDOW, h0 : h0 + HEAD_DIM] = a

    for i in range(sp - 1):
        @pl.when(i < me)
        def _():
            state_copy(1, i).wait_recv()

        @pl.when(i >= me)
        def _():
            state_in[i] = jnp.zeros(state_in.shape[1:], BF)

    for b in range(fs):
        half = (b % 2) * KEY_DIM
        incoming = jnp.zeros((VALUE_DIM, KEY_DIM), F32)
        for i in range(sp - 1):
            got = state_in[i, b // 2, :VALUE_DIM, half : half + KEY_DIM].astype(F32)
            kept = state_in[i, b // 2, VALUE_DIM : VALUE_DIM + 1, half : half + KEY_DIM].astype(F32)
            incoming = jnp.where(i < me, kept * incoming + got, incoming)
        o = local_out[b] + nt(q_far[b], incoming.astype(BF))
        hidden[b, :, :VALUE_DIM] = rms_rows(o, hgain_ref[...]).astype(BF)

    forward = 2 * me < sp
    nc = o_buf.shape[2]

    def chunk(t):
        return lax.rem(jnp.where(forward, me + t, me - t) + sp, sp)

    def half_copy(s):
        return remote(half_out.at[s], half_in.at[s], half_send.at[s], half_recv.at[s], {"tp": 1 - c})

    def piece_copy(s, d, target):
        return remote(
            piece_out.at[s, d - 1], piece_in.at[s, d - 1],
            piece_send.at[s, d - 1], piece_recv.at[s, d - 1], {"fs": target},
        )

    def produce(t):
        s = chunk(t)

        @pl.when(jnp.logical_not(inner) & (t > 0))
        def _():
            o_copy(s, 0, False).wait_recv()

        w = o_buf[s]
        for b in range(fs):
            part = nn(hidden[b], w)
            lo, hi = part[:own], part[own:]
            half_out[s, b] = jnp.where(c == 0, hi, lo).astype(BF)
            half_own[s, b] = jnp.where(c == 0, lo, hi)
        half_copy(s).start()

    def combine(t):
        s = chunk(t)
        half_copy(s).wait_recv()
        for d in range(1, fs):
            to = lax.rem(f + d, fs)
            piece_out[s, d - 1] = (half_own[s, to] + half_in[s, to].astype(F32)).astype(BF)
            piece_copy(s, d, to).start()
        piece_own[s] = half_own[s, f] + half_in[s, f].astype(F32)

    def finish(t):
        s = chunk(t)
        total = piece_own[s]
        for d in range(1, fs):
            piece_copy(s, d, f).wait_recv()
            total += piece_in[s, d - 1].astype(F32)
        if len(out_ref.shape) == 2:
            out_ref[:, pl.ds(pl.multiple_of(s * nc, nc), nc)] = total.astype(BF)
        else:
            out_ref[s] = total.astype(BF)

    produce(0)

    def steady(t, _):
        produce(t)
        combine(t - 1)
        return 0

    lax.fori_loop(1, sp, steady, 0)
    combine(sp - 1)

    def close(t, _):
        finish(t)
        s = chunk(t)
        half_copy(s).wait_send()
        for d in range(1, fs):
            piece_copy(s, d, f).wait_send()
        return 0

    lax.fori_loop(0, sp, close, 0)

    for k in range(sp - 1):
        @pl.when((me - k >= 0) & (me + 1 < sp))
        def _():
            l_copy(me - k, 0, False).wait_send()
            w_copy(me - k, 0, False).wait_send()
            o_copy(me - k, 0, False).wait_send()

        @pl.when((me + k < sp) & (me >= 1))
        def _():
            l_copy(me + k, 1, False).wait_send()
            w_copy(me + k, 1, False).wait_send()
            o_copy(me + k, 1, False).wait_send()

    for i in range(sp):
        @pl.when(i != me)
        def _():
            for copy in pair_copies(i, side):
                copy.wait_send()

    for d in range(1, plane):
        tok_copy(d, mine, mine).wait_send()

    @pl.when(me + 1 < sp)
    def _():
        edge.wait_send()

    for d in range(1, sp):
        @pl.when(me + d < sp)
        def _():
            state_copy(d, me).wait_send()


def per_device(
    tokens,
    norm_gain,
    gla_query_weight,
    gla_key_weight,
    gla_value_weight,
    decay_down,
    decay_up,
    decay_bias,
    head_gain,
    window_query_weight,
    window_key_weight,
    window_value_weight,
    sink_logit,
    gla_output_weight,
    window_output_weight,
):
    fs, tp, sp = (lax.axis_size(n) for n in ("fs", "tp", "sp"))
    low = decay_down.T
    own = tokens.shape[1]
    rows = own * tp
    kc = decay_down.shape[0]
    width = VALUE_DIM + 4 * HEAD_DIM + 2 * KEY_DIM
    rank = low.shape[0]
    depth = (gla_output_weight.shape[0] + window_output_weight.shape[0]) // fs
    nc = gla_output_weight.shape[1]
    flat = nc % 128 == 0
    vm = pltpu.VMEM
    dma = pltpu.SemaphoreType.DMA
    scratch = [
        vm((fs * rows, tokens.shape[2]), BF),
        vm((sp * kc, width), BF),
        vm((sp, rank, kc), BF),
        vm((sp, depth, nc), BF),
        vm((fs, rows, width + 128), BF),
        vm((fs, WINDOW, 2 * HEAD_DIM), BF),
        vm((fs, WINDOW, 2 * HEAD_DIM), BF),
        vm((fs // 2, VALUE_DIM + 16, 2 * KEY_DIM), BF),
        vm((sp, fs // 2, VALUE_DIM + 16, 2 * KEY_DIM), BF),
        vm((fs, rows, VALUE_DIM), F32),
        vm((fs, rows, KEY_DIM), BF),
        vm((fs, rows, depth), BF),
        vm((sp, fs, own, nc), BF),
        vm((sp, fs, own, nc), BF),
        vm((sp, fs, own, nc), F32),
        vm((sp, fs - 1, own, nc), BF),
        vm((sp, fs - 1, own, nc), BF),
        vm((sp, own, nc), F32),
        dma((6,)),
        dma((fs * tp - 1,)),
        dma((fs * tp - 1,)),
        dma((2, sp)),
        dma((sp,)),
        dma((2, sp)),
        dma((sp,)),
        dma((2, sp)),
        dma((sp,)),
        dma((sp,)),
        dma((sp,)),
        dma((sp,)),
        dma((sp,)),
        dma((2, sp)),
        dma((sp,)),
        dma((2,)),
        dma((sp,)),
        dma((sp,)),
        dma((sp,)),
        dma((sp,)),
        dma((sp, fs - 1)),
        dma((sp, fs - 1)),
    ]
    spec = pl.BlockSpec(memory_space=pltpu.VMEM)
    anywhere = pl.BlockSpec(memory_space=pl.ANY)
    mixed = pl.pallas_call(
        functools.partial(mixer_kernel, (sp, fs, tp)),
        out_shape=jax.ShapeDtypeStruct((own, sp * nc) if flat else (sp, own, nc), BF),
        in_specs=[
            anywhere if i in (1, 2, 8, 9) else spec for i in range(15)
        ],
        out_specs=spec,
        scratch_shapes=scratch,
        compiler_params=pltpu.CompilerParams(
            has_side_effects=True, vmem_limit_bytes=60 * 1024 * 1024
        ),
    )(
        tokens[0],
        gla_value_weight,
        window_query_weight,
        gla_query_weight,
        gla_key_weight,
        window_key_weight,
        window_value_weight,
        low,
        gla_output_weight,
        window_output_weight,
        norm_gain[None],
        decay_up,
        decay_bias[None],
        head_gain[None],
        sink_logit[None],
    )
    return (mixed if flat else mixed.transpose(1, 0, 2)).reshape(1, own, sp * nc)


def solution(mesh):
    in_specs = (
        P("fs", ("sp", "tp"), None),
        P(),
        P("sp", "tp"),
        P("sp", "tp"),
        P("sp", "tp"),
        P("sp", None),
        P(None, "tp"),
        P("tp"),
        P(),
        P("sp", "tp"),
        P("sp", "tp"),
        P("sp", "tp"),
        P("tp"),
        P("tp", "sp"),
        P("tp", "sp"),
    )
    out_specs = P("fs", ("sp", "tp"), None)
    return jax.shard_map(
        per_device, mesh=mesh, in_specs=in_specs, out_specs=out_specs, check_vma=False
    )
```
